256 devices in a mesh: rep: 2 (over z_hi), fs: 16 (over z_lo, y), tp: 8 (over x, core).
Axes of the slice: x: 4, y: 4, z: 8 (z_hi: 2, z_lo: 4; z = z_hi * 4 + z_lo), core: 2. Of those that a mesh axis runs over, the one named last changes fastest.
Arguments:
- tokens: bfloat16 [49152, 2048], P(('rep', 'fs', 'tp')), may hold values from -6 to 6
- mix_gain_in: float32 [2048], replicated, may hold values from 0.1 to 1.9
- pool_weight: bfloat16 [4, 512, 512], P(None, 'fs'), may hold values from -0.25 to 0.25
- mix_gain_out: float32 [2048], replicated, may hold values from 0.1 to 1.9
- ffn_gain_in: float32 [2048], replicated, may hold values from 0.1 to 1.9
- gate_weight: bfloat16 [2048, 5632], P('fs', 'tp'), may hold values from -0.125 to 0.125
- up_weight: bfloat16 [2048, 5632], P('fs', 'tp'), may hold values from -0.125 to 0.125
- gate_taps: float32 [3, 5632], replicated, may hold values from -3.5 to 3.5
- up_taps: float32 [3, 5632], replicated, may hold values from -3.5 to 3.5
- down_weight: bfloat16 [5632, 2048], P('tp', 'fs'), may hold values from -0.078125 to 0.078125
- ffn_gain_out: float32 [2048], replicated, may hold values from 0.1 to 1.9
Outputs:
- mixed_out: bfloat16 [49152, 2048], P(('rep', 'fs', 'tp'))
The draws below stay inside these ranges and needn't reach their ends.
All inputs are finite; a program needn't handle non-finite values.
Results may differ from the reference program's by a relative error of at most 0.014.
Values may be sent and summed in bfloat16 or wider, within the bound.
No kernel may reach another device: no remote copies, remote signals or barrier semaphores. Data moves between devices by JAX's collectives and lax.ppermute only.
A program may use at most 128 MiB of HBM per device.

```python
import jax
import jax.numpy as jnp
from jax import lax

D = 2048
FF = 5632
GROUPS = 4
CONV_WIDTH = 3
GC = 512
SEQ_LEN = 1536
SEQS = 32
TOKENS = 49152
N_TP = 8


def level_of(rng, dims, cuts, smallest, largest):
    level = 1.0
    for position, blocks in cuts:
        heights = jax.random.uniform(jax.random.fold_in(jax.random.fold_in(rng, 6), position), (blocks,), jnp.float32, smallest / len(cuts), largest / len(cuts))
        level = level * jnp.repeat(jnp.exp(heights), dims[position] // blocks).reshape((-1,) + (1,) * (len(dims) - 1 - position))
    return level


def bell_draw(own_key, dims, deviation, limit, cuts=(), kind=jnp.bfloat16):
    values = jax.random.normal(own_key, dims, jnp.float32) * deviation
    if len(cuts) > 0:
        values = level_of(own_key, dims, cuts, -0.22, 0.18) * values
    return jnp.clip(values, min=-limit, max=limit).astype(kind)


def setup_inputs(seed: int = 0) -> dict:
    key_of = jax.random.split(jax.random.key(seed), 12)
    return {
        "tokens": bell_draw(key_of[0], (TOKENS, D), 1.0, 6.0, ((0, 256),)),
        "mix_gain_in": jnp.clip(1.0 + 0.18 * jax.random.normal(key_of[1], (D,), jnp.float32), 0.1, 1.9),
        "pool_weight": bell_draw(key_of[2], (GROUPS, GC, GC), GC ** -0.5, 0.25, ((1, 16),)),
        "mix_gain_out": jnp.clip(1.0 + 0.18 * jax.random.normal(key_of[3], (D,), jnp.float32), 0.1, 1.9),
        "ffn_gain_in": jnp.clip(1.0 + 0.18 * jax.random.normal(key_of[4], (D,), jnp.float32), 0.1, 1.9),
        "gate_weight": bell_draw(key_of[5], (D, FF), D ** -0.5, 0.125, ((0, 16), (1, 8))),
        "up_weight": bell_draw(key_of[6], (D, FF), D ** -0.5, 0.125, ((0, 16), (1, 8))),
        "gate_taps": bell_draw(key_of[7], (CONV_WIDTH, FF), CONV_WIDTH ** -0.5, 3.5, (), jnp.float32),
        "up_taps": bell_draw(key_of[8], (CONV_WIDTH, FF), CONV_WIDTH ** -0.5, 3.5, (), jnp.float32),
        "down_weight": bell_draw(key_of[9], (FF, D), FF ** -0.5, 0.078125, ((0, 8), (1, 16))),
        "ffn_gain_out": jnp.clip(1.0 + 0.18 * jax.random.normal(key_of[10], (D,), jnp.float32), 0.1, 1.9),
    }


pool_spans = (2, 4, 8, 16)
rms_eps = 1e-06

def rms_scale(values, gain):
    floats = values.astype(jnp.float32)
    return floats * lax.rsqrt(lax.optimization_barrier(jnp.mean(floats * floats, axis=-1, keepdims=True)) + rms_eps) * gain.astype(jnp.float32)

def pooled_gap(padded, first, count):
    margin = padded.shape[0] - count
    floats = padded.astype(jnp.float32)
    width = padded.shape[1] // len(pool_spans)
    where = first + jnp.arange(count, dtype=jnp.int32)
    pieces = []
    for group, span in enumerate(pool_spans):
        block = floats[:, group * width:(group + 1) * width]
        total = jnp.zeros((count, width), jnp.float32)
        for back in range(span):
            total = total + block[margin - back:margin - back + count]
        divisor = jnp.minimum(where + 1, span).astype(jnp.float32)
        pieces.append(total / divisor[:, None] - block[margin:])
    return jnp.concatenate(pieces, axis=1).astype(jnp.bfloat16)

def causal_taps(pre, taps):
    width = taps.shape[0]
    floats = pre.astype(jnp.float32)
    padded = jnp.concatenate([jnp.zeros((width - 1, pre.shape[1]), jnp.float32), floats], axis=0)
    total = jnp.zeros(floats.shape, jnp.float32)
    for offset in range(width):
        total = total + taps[offset].astype(jnp.float32) * padded[offset:offset + pre.shape[0]]
    return total

def reference(tokens, mix_gain_in, pool_weight, mix_gain_out, ffn_gain_in, gate_weight, up_weight, gate_taps, up_taps, down_weight, ffn_gain_out):
    margin = max(pool_spans) - 1

    def one_sequence(rows):
        normed = rms_scale(rows, mix_gain_in).astype(jnp.bfloat16)
        padded = jnp.concatenate([jnp.zeros((margin, D), jnp.bfloat16), normed], axis=0)
        gap = pooled_gap(padded, 0, SEQ_LEN)
        mixed = jnp.einsum('rgc,gcj->rgj', gap.reshape(SEQ_LEN, GROUPS, GC).astype(jnp.float32), pool_weight.astype(jnp.float32))
        mixed = mixed.reshape(SEQ_LEN, D).astype(jnp.bfloat16)
        after_mix = rows.astype(jnp.float32) + rms_scale(mixed, mix_gain_out)
        channel_in = rms_scale(after_mix, ffn_gain_in).astype(jnp.bfloat16)
        gate_pre = jnp.dot(channel_in, gate_weight, preferred_element_type=jnp.float32).astype(jnp.bfloat16)
        up_pre = jnp.dot(channel_in, up_weight, preferred_element_type=jnp.float32).astype(jnp.bfloat16)
        gate_conv = causal_taps(gate_pre, gate_taps)
        up_conv = causal_taps(up_pre, up_taps)
        hidden = (jax.nn.gelu(gate_conv, approximate=True) * up_conv).astype(jnp.bfloat16)
        partial_value = jnp.einsum('rtf,tfd->rtd', hidden.reshape(SEQ_LEN, N_TP, FF // N_TP).astype(jnp.float32), down_weight.reshape(N_TP, FF // N_TP, D).astype(jnp.float32)).astype(jnp.bfloat16)
        channel_out = lax.optimization_barrier(jnp.sum(partial_value.astype(jnp.float32), axis=1))
        return (after_mix + rms_scale(channel_out, ffn_gain_out)).astype(jnp.bfloat16)
    result = lax.map(one_sequence, tokens.reshape(SEQS, SEQ_LEN, D))
    return result.reshape(TOKENS, D)
```

```python
import jax
import jax.numpy as jnp
from jax import lax
from jax.experimental import pallas as pl
from jax.experimental.pallas import tpu as pltpu
from jax.sharding import PartitionSpec as P


pool_spans = (2, 4, 8, 16)
rms_eps = 1e-06
AXES = ("rep", "fs", "tp")
RING = 4
CORES = 2
REPS = 2
HALO = 16
BF16 = jnp.bfloat16
F32 = jnp.float32
STEPS = (0, -1, 1, 2)


def flat(z, y, x, c):
    return ((z * RING + y) * RING + x) * CORES + c


def permutation(move):
    pairs = []
    for z in range(REPS * RING):
        for y in range(RING):
            for x in range(RING):
                for c in range(CORES):
                    dz, dy, dx, dc = move(z, c)
                    there = flat((z + dz) % (REPS * RING), (y + dy) % RING, (x + dx) % RING, (c + dc) % CORES)
                    pairs.append((flat(z, y, x, c), there))
    return pairs


def along(first, step):
    def move(z, c):
        on_y = (c == 0) == first
        if on_y:
            return (0, step, 0, 0)
        if step == 2:
            return (2 if z % 2 == 0 else -2, 0, 0, 0)
        return (step, 0, 0, 0)

    return permutation(move)


F_UP, F_DOWN, F_FAR = along(True, 1), along(True, -1), along(True, 2)
G_UP, G_DOWN, G_FAR = along(False, 1), along(False, -1), along(False, 2)
X_UP = permutation(lambda z, c: (0, 0, 1, 0))
X_DOWN = permutation(lambda z, c: (0, 0, -1, 0))
X_FAR = permutation(lambda z, c: (0, 0, 2, 0))
SWAP = permutation(lambda z, c: (0, 0, 0, 1))
NEXT_ROWS = permutation(lambda z, c: (0, 0, 0, 1) if c == 0 else (0, 0, 1, 1))


def sent(a, pairs):
    return lax.ppermute(a, AXES, pairs)


def gathered_pairs(w):
    r1 = sent(w, F_UP)
    r3 = sent(w, F_DOWN)
    r2 = sent(w, F_FAR)
    near = jnp.stack([w, r1])
    far = jnp.stack([r3, r2])
    a1 = sent(near, G_UP)
    a3 = sent(near, G_DOWN)
    b1 = sent(far, G_UP)
    b3 = sent(far, G_DOWN)
    a2 = sent(a1, G_UP)
    b2 = sent(b3, G_DOWN)
    return [near, far, a1, a3, b1, b3, a2, b2]


PAIR_OFFSETS = [
    ((0, 0), (-1, 0)),
    ((1, 0), (2, 0)),
    ((0, -1), (-1, -1)),
    ((0, 1), (-1, 1)),
    ((1, -1), (2, -1)),
    ((1, 1), (2, 1)),
    ((0, 2), (-1, 2)),
    ((1, 2), (2, 2)),
]
FLAT_OFFSETS = [o for pair in PAIR_OFFSETS for o in pair]
POOL_OFFSETS = [(f, g) for g in STEPS for f in STEPS]


def absolute(offsets, core):
    fs = lax.axis_index("fs")
    z, y = fs // RING, fs % RING
    df = jnp.array([o[0] for o in offsets], jnp.int32)
    dg = jnp.array([o[1] for o in offsets], jnp.int32)
    by_y = ((z + dg) % RING) * RING + (y + df) % RING
    by_z = ((z + df) % RING) * RING + (y + dg) % RING
    return jnp.where(core == 0, by_y, by_z).astype(jnp.int32)


def whole(space=pltpu.VMEM):
    return pl.BlockSpec(memory_space=space)


def roll_rows(a, shift):
    return pltpu.roll(a, shift, 0)


def gap_kernel(tp_ref, tokens_ref, halo_ref, gain_ref, gap_ref, padded):
    rows, features = tokens_ref.shape
    width = features // len(pool_spans)
    tp = tp_ref[0]
    gain = gain_ref[...]

    def normed(block):
        floats = block.astype(F32)
        scale = lax.rsqrt(jnp.mean(floats * floats, axis=-1, keepdims=True) + rms_eps)
        return (floats * scale * gain).astype(BF16).astype(F32)

    before = normed(halo_ref[...])
    padded[0:HALO, :] = jnp.where(tp > 0, before, 0.0)
    chunk = 32

    def fill(i, carry):
        start = pl.multiple_of(i * chunk, chunk)
        padded[pl.ds(HALO + start, chunk), :] = normed(tokens_ref[pl.ds(start, chunk), :])
        return carry

    lax.fori_loop(0, rows // chunk, fill, 0)

    def pool(i, carry):
        start = pl.multiple_of(i * chunk, chunk)
        where = tp * rows + start + lax.broadcasted_iota(jnp.int32, (chunk, 1), 0)
        for group, span in enumerate(pool_spans):
            block = padded[pl.ds(start, chunk + HALO), group * width : (group + 1) * width]
            total = block
            step = 1
            while step < span:
                total = total + roll_rows(total, step)
                step *= 2
            inverse = 1.0 / jnp.minimum(where + 1, span).astype(F32)
            gap = total[HALO:] * inverse - block[HALO:]
            gap_ref[pl.ds(start, chunk), group * width : (group + 1) * width] = gap.astype(BF16)
        return carry

    lax.fori_loop(0, rows // chunk, pool, 0)


def mix_kernel(
    table_ref, gap_ref, tokens_ref, own_ref, other_ref, gain_out_ref, gain_in_ref, after_ref, channel_ref, pool, mixed, sems
):
    rows, features = tokens_ref.shape
    groups = pool.shape[0]
    width = features // groups
    half = groups // CORES
    part = own_ref.shape[2]
    core = lax.rem(table_ref[0], CORES)
    copies = []
    for which, ref in enumerate((own_ref, other_ref)):
        first = half * (core if which == 0 else 1 - core)
        for k in range(RING * RING):
            at = pl.multiple_of(table_ref[1 + which * RING * RING + k] * part, part)
            copy = pltpu.make_async_copy(
                ref.at[k], pool.at[pl.ds(first, half), pl.ds(at, part), :], sems.at[which * RING * RING + k]
            )
            copy.start()
            copies.append(copy)
    for copy in copies:
        copy.wait()
    for g in range(groups):
        product = jnp.dot(gap_ref[:, g * width : (g + 1) * width], pool[g], preferred_element_type=F32)
        mixed[:, g * width : (g + 1) * width] = product.astype(BF16)
    gain_out = gain_out_ref[...]
    gain_in = gain_in_ref[...]
    chunk = 32

    def scaled(floats, gain):
        return floats * lax.rsqrt(jnp.mean(floats * floats, axis=-1, keepdims=True) + rms_eps) * gain

    def norms(i, carry):
        at = pl.ds(pl.multiple_of(i * chunk, chunk), chunk)
        after = tokens_ref[at, :].astype(F32) + scaled(mixed[at, :].astype(F32), gain_out)
        after_ref[at, :] = after
        channel_ref[at, :] = scaled(after, gain_in).astype(BF16)
        return carry

    lax.fori_loop(0, rows // chunk, norms, 0)


def ffn_kernel(table_ref, *refs):
    rows, features, units, both = 192, 2048, 704, 1408
    x_refs, refs = refs[:10], refs[10:]
    w_refs, refs = refs[:8], refs[8:]
    d_refs, refs = refs[:8], refs[8:]
    taps_ref, own_ref, sib_ref, xv, wv, dv, pre, hv, x_sems, w_sems, d_sems = refs
    tp = table_ref[0]
    chip, core = tp // CORES, lax.rem(tp, CORES)
    part = w_refs[0].shape[1]
    lanes = d_refs[0].shape[2]

    copies_w, copies_d, copies_x = [], [], []
    for k in range(RING * RING):
        at = table_ref[1 + k]
        copies_w.append(
            pltpu.make_async_copy(
                w_refs[k // 2].at[k % 2], wv.at[pl.ds(pl.multiple_of(at * part, part), part), :], w_sems.at[k]
            )
        )
        copies_d.append(
            pltpu.make_async_copy(
                d_refs[k // 2].at[k % 2],
                dv.at[pl.ds(0, units), pl.ds(pl.multiple_of(at * lanes, lanes), lanes)],
                d_sems.at[k],
            )
        )
    for k in range(6):
        copies_x.append(pltpu.make_async_copy(x_refs[k], xv.at[k], x_sems.at[k]))
    half = rows // 2
    for k in range(4):
        copies_x.append(
            pltpu.make_async_copy(x_refs[6 + k], xv.at[6 + k // 2, pl.ds((k % 2) * half, half), :], x_sems.at[6 + k])
        )
    for copy in copies_w + copies_x + copies_d:
        copy.start()
    pre[0:8, :] = jnp.zeros((8, both), F32)
    dv[units:, :] = jnp.zeros((dv.shape[0] - units, features), BF16)
    hv[...] = jnp.zeros(hv.shape, BF16)
    for copy in copies_w + copies_x:
        copy.wait()

    def block_of(k):
        place, other = k // 2, lax.rem(k, 2)
        step = jnp.where(place == 0, 0, jnp.where(place == 1, RING - 1, place - 1))
        return lax.rem(chip + step, RING) * CORES + lax.rem(core + other, CORES)

    def project(k, carry):
        at = pl.multiple_of(8 + block_of(k) * rows, 8)
        product = jnp.dot(xv[k], wv[...], preferred_element_type=F32)
        pre[pl.ds(at, rows), :] = product.astype(BF16).astype(F32)
        return carry

    lax.fori_loop(0, 2 * RING, project, 0)
    for copy in copies_d:
        copy.wait()

    def conv(at, col):
        block = pre[pl.ds(at, rows + 8), col : col + 128]
        taps = taps_ref[:, col : col + 128]
        total = taps[2:3] * block + taps[1:2] * roll_rows(block, 1) + taps[0:1] * roll_rows(block, 2)
        return total[8:]

    def gated(k):
        at = pl.multiple_of(block_of(k) * rows, 8)
        for tile in range(5):
            gate = conv(at, tile * 128)
            up = conv(at, 768 + tile * 128)
            hv[:, tile * 128 : (tile + 1) * 128] = (jax.nn.gelu(gate, approximate=True) * up).astype(BF16)
        both_halves = conv(at, 640)
        up = pltpu.roll(both_halves, 64, 1)
        last = (jax.nn.gelu(both_halves, approximate=True) * up).astype(BF16)
        hv[:, 640:704] = last[:, :64]

    def down(k, carry):
        gated(k)
        product = jnp.dot(hv[...], dv[...], preferred_element_type=F32).astype(BF16)
        place = k // 2

        @pl.when(lax.rem(k, 2) == 0)
        def _():
            own_ref[place] = product

        @pl.when(lax.rem(k, 2) == 1)
        def _():
            sib_ref[place] = product

        return carry

    lax.fori_loop(0, 2 * RING, down, 0)


def add_kernel(own_ref, sib_ref, *out_refs):
    for k, out in enumerate(out_refs):
        out[...] = (own_ref[k].astype(F32) + sib_ref[k].astype(F32)).astype(BF16)


def final_kernel(after_ref, a_ref, b_ref, c_ref, d_ref, gain_ref, out_ref):
    gain = gain_ref[...]
    chunk = 32

    def step(i, carry):
        at = pl.ds(pl.multiple_of(i * chunk, chunk), chunk)
        total = (a_ref[at, :].astype(F32) + b_ref[at, :].astype(F32)) + (c_ref[at, :].astype(F32) + d_ref[at, :].astype(F32))
        scale = lax.rsqrt(jnp.mean(total * total, axis=-1, keepdims=True) + rms_eps)
        out_ref[at, :] = (after_ref[at, :] + total * scale * gain).astype(BF16)
        return carry

    lax.fori_loop(0, after_ref.shape[0] // chunk, step, 0)


def kept(limit=None):
    return pltpu.CompilerParams(vmem_limit_bytes=limit) if limit else None


def cost(flops, size):
    return pl.CostEstimate(flops=int(flops), bytes_accessed=int(size), transcendentals=0)


def arranged(gate, up):
    return jnp.concatenate([gate[:, :640], gate[:, 640:], up[:, 640:], up[:, :640]], axis=1)


def shards(
    tokens,
    mix_gain_in,
    pool_weight,
    mix_gain_out,
    ffn_gain_in,
    gate_weight,
    up_weight,
    gate_taps,
    up_taps,
    down_weight,
    ffn_gain_out,
):
    rows, features = tokens.shape
    groups, part, width = pool_weight.shape
    units = gate_weight.shape[1]
    tp = lax.axis_index("tp")
    core = tp % CORES
    tp_only = tp.astype(jnp.int32).reshape(1)
    mix_table = jnp.concatenate([tp_only, absolute(POOL_OFFSETS, core), absolute(POOL_OFFSETS, 1 - core)])
    ffn_table = jnp.concatenate([tp_only, absolute(FLAT_OFFSETS, core)])

    halo = sent(tokens[rows - HALO :], NEXT_ROWS)
    half = groups // CORES
    mine = lax.dynamic_slice_in_dim(pool_weight, core * half, half, 0)
    q1, q3, q2 = sent(mine, F_UP), sent(mine, F_DOWN), sent(mine, F_FAR)
    line = jnp.stack([mine, q1, q3, q2])
    plane = jnp.concatenate([line, sent(line, G_UP), sent(line, G_DOWN), sent(line, G_FAR)])
    other_plane = sent(plane, SWAP)

    gate_up = gathered_pairs(arranged(gate_weight, up_weight))
    downs = gathered_pairs(down_weight)

    gap = pl.pallas_call(
        gap_kernel,
        out_shape=jax.ShapeDtypeStruct((rows, features), BF16),
        in_specs=[whole(pltpu.SMEM), whole(), whole(), whole()],
        out_specs=whole(),
        scratch_shapes=[pltpu.VMEM((rows + HALO, features), F32)],
        cost_estimate=cost(3e9, 1.6e6),
        name="gap",
    )(tp_only, tokens, halo, mix_gain_in.reshape(1, features))

    after, channel = pl.pallas_call(
        mix_kernel,
        out_shape=(jax.ShapeDtypeStruct((rows, features), F32), jax.ShapeDtypeStruct((rows, features), BF16)),
        in_specs=[whole(pltpu.SMEM), whole(), whole(), whole(pl.ANY), whole(pl.ANY), whole(), whole()],
        out_specs=(whole(), whole()),
        scratch_shapes=[
            pltpu.VMEM((groups, width, width), BF16),
            pltpu.VMEM((rows, features), BF16),
            pltpu.SemaphoreType.DMA((2 * RING * RING,)),
        ],
        cost_estimate=cost(4e9, 6e6),
        name="mix",
    )(mix_table, gap, tokens, plane, other_plane, mix_gain_out.reshape(1, features), ffn_gain_in.reshape(1, features))

    from_left, from_right = sent(channel, X_UP), sent(channel, X_DOWN)
    far_top = sent(from_left[: rows // 2], X_UP)
    far_bottom = sent(from_right[rows // 2 :], X_DOWN)
    x_list = []
    for a in (channel, from_left, from_right):
        x_list += [a, sent(a, SWAP)]
    x_list += [far_top, far_bottom, sent(far_top, SWAP), sent(far_bottom, SWAP)]

    def taps_of(taps):
        return lax.dynamic_slice_in_dim(taps, tp * units, units, 1)

    taps = arranged(taps_of(gate_taps), taps_of(up_taps))
    own, sib = pl.pallas_call(
        ffn_kernel,
        out_shape=(jax.ShapeDtypeStruct((RING, rows, features), BF16),) * 2,
        in_specs=[whole(pltpu.SMEM)] + [whole(pl.ANY)] * 26 + [whole()],
        out_specs=(whole(), whole()),
        scratch_shapes=[
            pltpu.VMEM((2 * RING, rows, features), BF16),
            pltpu.VMEM((features, 2 * units), BF16),
            pltpu.VMEM((768, features), BF16),
            pltpu.VMEM((2 * RING * rows + 8, 2 * units), F32),
            pltpu.VMEM((rows, 768), BF16),
            pltpu.SemaphoreType.DMA((10,)),
            pltpu.SemaphoreType.DMA((16,)),
            pltpu.SemaphoreType.DMA((16,)),
        ],
        cost_estimate=cost(14e9, 2.4e7),
        compiler_params=kept(52 * 2**20),
        name="ffn",
    )(ffn_table, *x_list, *gate_up, *downs, taps)

    sums = pl.pallas_call(
        add_kernel,
        out_shape=(jax.ShapeDtypeStruct((rows, features), BF16),) * RING,
        in_specs=[whole(), whole()],
        out_specs=(whole(),) * RING,
        cost_estimate=cost(1e9, 9e6),
        name="add",
    )(own, sent(sib, SWAP))
    got = (sent(sums[2], X_UP), sent(sums[1], X_DOWN), sent(sums[3], X_FAR))
    return pl.pallas_call(
        final_kernel,
        out_shape=jax.ShapeDtypeStruct((rows, features), BF16),
        in_specs=[whole()] * 6,
        out_specs=whole(),
        cost_estimate=cost(2e9, 6e6),
        name="final",
    )(after, sums[0], *got, ffn_gain_out.reshape(1, features))


def solution(mesh):
    in_specs = (
        P(("rep", "fs", "tp"), None),
        P(),
        P(None, "fs", None),
        P(),
        P(),
        P("fs", "tp"),
        P("fs", "tp"),
        P(),
        P(),
        P("tp", "fs"),
        P(),
    )
    out_specs = P(("rep", "fs", "tp"), None)
    return jax.shard_map(shards, mesh=mesh, in_specs=in_specs, out_specs=out_specs, check_vma=False)
```

```python
import functools

import jax
import jax.numpy as jnp
from jax import lax
from jax.experimental import pallas as pl
from jax.experimental.pallas import tpu as pltpu
from jax.sharding import PartitionSpec as P


pool_spans = (2, 4, 8, 16)
rms_eps = 1e-06
AXES = ("rep", "fs", "tp")
RING = 4
CORES = 2
REPS = 2
HALO = 16
BF16 = jnp.bfloat16
F32 = jnp.float32
STEPS = (0, -1, 1, 2)


def flat(z, y, x, c):
    return ((z * RING + y) * RING + x) * CORES + c


def permutation(move):
    pairs = []
    for z in range(REPS * RING):
        for y in range(RING):
            for x in range(RING):
                for c in range(CORES):
                    dz, dy, dx, dc = move(z, c)
                    there = flat((z + dz) % (REPS * RING), (y + dy) % RING, (x + dx) % RING, (c + dc) % CORES)
                    pairs.append((flat(z, y, x, c), there))
    return pairs


def along(first, step):
    def move(z, c):
        on_y = (c == 0) == first
        if on_y:
            return (0, step, 0, 0)
        if step == 2:
            return (2 if z % 2 == 0 else -2, 0, 0, 0)
        return (step, 0, 0, 0)

    return permutation(move)


F_UP, F_DOWN, F_FAR = along(True, 1), along(True, -1), along(True, 2)
G_UP, G_DOWN, G_FAR = along(False, 1), along(False, -1), along(False, 2)
X_ONE = permutation(lambda z, c: (0, 0, 1 if c == 0 else -1, 0))
X_TWO = permutation(lambda z, c: (0, 0, -1 if c == 0 else 1, 0))
X_UP = permutation(lambda z, c: (0, 0, 1, 0))
X_DOWN = permutation(lambda z, c: (0, 0, -1, 0))
SWAP = permutation(lambda z, c: (0, 0, 0, 1))
NEXT_ROWS = permutation(lambda z, c: (0, 0, 0, 1) if c == 0 else (0, 0, 1, 1))


def sent(a, pairs):
    return lax.ppermute(a, AXES, pairs)


def gathered_lines(w):
    r1 = sent(w, F_UP)
    r3 = sent(w, F_DOWN)
    r2 = sent(w, F_FAR)
    line = jnp.stack([w, r1, r3, r2])
    return [line, sent(line, G_UP), sent(line, G_DOWN), sent(line, G_FAR)]


LINE_OFFSETS = [(f, g) for g in STEPS for f in STEPS]
LINE_AT, OTHER_AT, TABLE = 1, 17, 33


def table_of():
    fs, tp = lax.axis_index("fs"), lax.axis_index("tp")
    z, y = fs // RING, fs % RING
    offsets = [(0, 0)] + LINE_OFFSETS + LINE_OFFSETS
    df = jnp.array([o[0] for o in offsets], jnp.int32)
    dg = jnp.array([o[1] for o in offsets], jnp.int32)
    place = jnp.arange(TABLE, dtype=jnp.int32)
    core = (tp + jnp.where(place >= OTHER_AT, 1, 0)) % CORES
    by_y = ((z + dg) % RING) * RING + (y + df) % RING
    by_z = ((z + df) % RING) * RING + (y + dg) % RING
    return jnp.where(place == 0, tp, jnp.where(core == 0, by_y, by_z)).astype(jnp.int32)


def whole(space=pltpu.VMEM):
    return pl.BlockSpec(memory_space=space)


def roll_rows(a, shift):
    return pltpu.roll(a, shift, 0)


def prepare_kernel(table_ref, pool_ref, gate_ref, up_ref, tokens_ref, mine_ref, piece_ref, end_ref, sems):
    half = mine_ref.shape[0]
    core = lax.rem(table_ref[0], CORES)
    units = gate_ref.shape[0]
    copies = [
        pltpu.make_async_copy(pool_ref.at[pl.ds(core * half, half)], mine_ref, sems.at[0]),
        pltpu.make_async_copy(gate_ref, piece_ref.at[pl.ds(0, units), :], sems.at[1]),
        pltpu.make_async_copy(up_ref, piece_ref.at[pl.ds(units, units), :], sems.at[2]),
        pltpu.make_async_copy(tokens_ref.at[pl.ds(tokens_ref.shape[0] - HALO, HALO), :], end_ref, sems.at[3]),
    ]
    start_all(copies)
    wait_all(copies)


def gap_kernel(tp_ref, tokens_ref, halo_ref, gain_ref, gate_taps_ref, up_taps_ref, gap_ref, kept_ref, padded):
    lanes = TILES * 128
    units = gate_taps_ref.shape[1] // (RING * CORES)
    start = tp_ref[0] * units
    ahead = lax.rem(start, 128)
    window = pl.ds(pl.multiple_of(start - ahead, 128), lanes)
    for n, ref in enumerate((gate_taps_ref, up_taps_ref)):
        taps = ref[:, window]
        kept_ref[:, n * lanes : (n + 1) * lanes] = jnp.where(ahead > 0, pltpu.roll(taps, lanes - 64, 1), taps)
    rows, features = tokens_ref.shape
    width = features // len(pool_spans)
    tp = tp_ref[0]
    gain = gain_ref[...]

    def normed(block):
        floats = block.astype(F32)
        scale = lax.rsqrt(jnp.mean(floats * floats, axis=-1, keepdims=True) + rms_eps)
        return (floats * scale * gain).astype(BF16).astype(F32)

    before = normed(halo_ref[...])
    padded[0:HALO, :] = jnp.where(tp > 0, before, 0.0)
    chunk = 32

    def fill(i, carry):
        start = pl.multiple_of(i * chunk, chunk)
        padded[pl.ds(HALO + start, chunk), :] = normed(tokens_ref[pl.ds(start, chunk), :])
        return carry

    lax.fori_loop(0, rows // chunk, fill, 0)

    def pool(i, carry):
        start = pl.multiple_of(i * chunk, chunk)
        where = tp * rows + start + lax.broadcasted_iota(jnp.int32, (chunk, 1), 0)
        for group, span in enumerate(pool_spans):
            block = padded[pl.ds(start, chunk + HALO), group * width : (group + 1) * width]
            total = block
            step = 1
            while step < span:
                total = total + roll_rows(total, step)
                step *= 2
            inverse = 1.0 / jnp.minimum(where + 1, span).astype(F32)
            gap = total[HALO:] * inverse - block[HALO:]
            gap_ref[pl.ds(start, chunk), group * width : (group + 1) * width] = gap.astype(BF16)
        return carry

    lax.fori_loop(0, rows // chunk, pool, 0)


def mix_kernel(table_ref, gap_ref, tokens_ref, *refs):
    lines, others, refs = refs[:RING], refs[RING : 2 * RING], refs[2 * RING :]
    gain_out_ref, gain_in_ref, after_ref, channel_ref, pool, mixed, sems = refs
    rows, features = tokens_ref.shape
    groups = pool.shape[0]
    width = features // groups
    half = groups // CORES
    part = lines[0].shape[2]
    core = lax.rem(table_ref[0], CORES)

    def piece(which, line, k):
        first = half * (core if which == 0 else 1 - core)
        at = table_ref[(LINE_AT if which == 0 else OTHER_AT) + line * RING + k]
        return pltpu.make_async_copy(
            (lines, others)[which][line].at[k],
            pool.at[pl.ds(first, half), pl.ds(pl.multiple_of(at * part, part), part), :],
            sems.at[(which * RING + line) * RING + k],
        )

    def each(act):
        for which in range(CORES):
            for line in range(RING):

                def step(k, carry, which=which, line=line):
                    act(piece(which, line, k))
                    return carry

                lax.fori_loop(0, RING, step, 0)

    each(lambda copy: copy.start())
    each(lambda copy: copy.wait())

    for g in range(groups):
        columns = slice(g * width, (g + 1) * width)
        mixed[:, columns] = jnp.dot(gap_ref[:, columns], pool[g], preferred_element_type=F32).astype(BF16)
    gain_out = gain_out_ref[...]
    gain_in = gain_in_ref[...]
    chunk = 32

    def scaled(floats, gain):
        return floats * lax.rsqrt(jnp.mean(floats * floats, axis=-1, keepdims=True) + rms_eps) * gain

    def norms(i, carry):
        at = pl.ds(pl.multiple_of(i * chunk, chunk), chunk)
        after = tokens_ref[at, :].astype(F32) + scaled(mixed[at, :].astype(F32), gain_out)
        after_ref[at, :] = after
        channel_ref[at, :] = scaled(after, gain_in).astype(BF16)
        return carry

    lax.fori_loop(0, rows // chunk, norms, 0)


PARTS = 2
TILES = 6


def start_all(copies):
    for copy in copies:
        copy.start()


def wait_all(copies):
    for copy in copies:
        copy.wait()


class Pieces:
    def __init__(self, table_ref, p_refs, first, count, fv, sems):
        self.table_ref, self.p_refs, self.first, self.count, self.fv, self.sems = table_ref, p_refs, first, count, fv, sems

    def copy(self, ref, line, k):
        lanes = ref.shape[2]
        rows = pl.ds(self.first, self.count)
        at = pl.multiple_of(self.table_ref[LINE_AT + line * RING + k] * lanes, lanes)
        return pltpu.make_async_copy(
            ref.at[k, rows, :], self.fv.at[rows, pl.ds(at, lanes)], self.sems.at[line * RING + k]
        )

    def start(self):
        for line, ref in enumerate(self.p_refs):

            def step(k, carry, line=line, ref=ref):
                self.copy(ref, line, k).start()
                return carry

            lax.fori_loop(0, RING, step, 0)

    def wait(self):
        for line, ref in enumerate(self.p_refs):

            def step(k, carry, line=line, ref=ref):
                self.copy(ref, line, k).wait()
                return carry

            lax.fori_loop(0, RING, step, 0)


def branch_product(xv, fv, branch, units):
    rows = pl.ds(pl.multiple_of(branch * units, 16), units)
    return lax.dot_general(xv, fv[rows, :], (((1,), (1,)), ((), ())), preferred_element_type=F32).astype(BF16)


def project_kernel(table_ref, here, here2, one, one2, two, two2, *refs):
    p_refs, refs = refs[:RING], refs[RING:]
    out, xv, fv, kept, x_sems, p_sems, o_sems = refs
    core = lax.rem(table_ref[0], CORES)
    units = fv.shape[0] // 2
    rows = one.shape[0]
    count = out.shape[0]
    places = [(core, core), (1 - core, 1 - core), (1 - core, core), (core, 1 - core)]
    copies = []
    for k, (ref, (slot, which)) in enumerate(zip((one, one2, two, two2), places)):
        at = pl.multiple_of(which * rows, rows)
        copies.append(pltpu.make_async_copy(ref, xv.at[slot, pl.ds(at, rows), :], x_sems.at[k]))

    def end_copies(ref):
        end = ref.at[pl.ds(rows - HALO, HALO), :]
        at = pl.ds(CORES * rows, HALO)
        return [pltpu.make_async_copy(end, xv.at[n, at, :], x_sems.at[4 + n]) for n in range(count)]

    @pl.when(core == 1)
    def _():
        start_all(end_copies(here))

    @pl.when(core == 0)
    def _():
        start_all(end_copies(here2))

    gates = Pieces(table_ref, p_refs, 0, units, fv, p_sems.at[0])
    ups = Pieces(table_ref, p_refs, units, units, fv, p_sems.at[1])

    def flush(n, branch):
        tiles = pl.ds(branch * TILES, TILES)
        return pltpu.make_async_copy(kept.at[n, tiles], out.at[n, tiles], o_sems.at[n, branch])

    start_all(copies)
    gates.start()
    wait_all(copies)
    wait_all(end_copies(here))
    gates.wait()
    ups.start()

    def step(i, carry):
        branch, n = i // count, lax.rem(i, count)

        @pl.when(i == count)
        def _():
            ups.wait()

        block = branch_product(xv[n], fv, branch, units)
        for t in range(TILES):
            part = block[:, t * 128 : min((t + 1) * 128, units)]
            kept[n, branch * TILES + t, :, 0 : part.shape[1]] = part
        flush(n, branch).start()
        return carry

    lax.fori_loop(0, 2 * count, step, 0)
    for n in range(count):
        for branch in range(2):
            flush(n, branch).wait()


def gated(pre, taps_ref, hv):
    rows = hv.shape[0]

    def conv(tile):
        taps = taps_ref[:, pl.ds(pl.multiple_of(tile * 128, 128), 128)]
        return (
            taps[2:3] * pre[tile, 8 : 8 + rows, :]
            + taps[1:2] * pre[tile, 7 : 7 + rows, :]
            + taps[0:1] * pre[tile, 6 : 6 + rows, :]
        )

    lane = lax.broadcasted_iota(jnp.int32, (1, 128), 1)

    def tile(n, carry):
        hidden = jax.nn.gelu(conv(n), approximate=True) * conv(TILES + n)
        valid = lane < jnp.where(n == TILES - 1, 64, 128)
        hv[:, pl.ds(pl.multiple_of(n * 128, 128), 128)] = jnp.where(valid, hidden, 0.0).astype(BF16)
        return carry

    lax.fori_loop(0, TILES, tile, 0)


def opened(first, tail, pre):
    def step(n, carry):
        before = tail[n].astype(F32)[8:]
        pre[n, 0:8, :] = jnp.where(first, 0.0, before)
        return carry

    lax.fori_loop(0, 2 * TILES, step, 0)


def out_copies(core, pv, own_ref, sib_ref, sems):
    rows = own_ref.shape[0]
    return [
        pltpu.make_async_copy(pv.at[pl.ds(pl.multiple_of((1 - core) * rows, rows), rows), :], sib_ref, sems.at[1]),
        pltpu.make_async_copy(pv.at[pl.ds(pl.multiple_of(core * rows, rows), rows), :], own_ref, sems.at[0]),
    ]


def down_product(hv, dv):
    return jnp.dot(hv[...], dv[...], preferred_element_type=F32).astype(BF16)


def cleared(dv, units):
    dv[units:, :] = jnp.zeros((dv.shape[0] - units, dv.shape[1]), BF16)


def last_kernel(step, before, parts, table_ref, own_x, sib_x, *refs):
    p_refs, refs = refs[:RING], refs[RING:]
    taps_ref, pre_ref, hv, end_ref, xv, fv, pre, tail, x_sems, p_sems, o_sems = refs
    tp = table_ref[0]
    chip, core = tp // CORES, lax.rem(tp, CORES)
    rows = own_x.shape[0]
    units = fv.shape[0] // 2
    length = hv.shape[0]
    ends = [pltpu.make_async_copy(pre_ref.at[before, :, pl.ds(length - 16, 16), :], tail, o_sems.at[0])]
    copies = [
        pltpu.make_async_copy(own_x, xv.at[pl.ds(pl.multiple_of(core * rows, rows), rows), :], x_sems.at[0]),
        pltpu.make_async_copy(sib_x, xv.at[pl.ds(pl.multiple_of((1 - core) * rows, rows), rows), :], x_sems.at[1]),
    ]
    gates = Pieces(table_ref, p_refs, 0, units, fv, p_sems.at[0])
    ups = Pieces(table_ref, p_refs, units, units, fv, p_sems.at[1])
    start_all(copies)
    gates.start()
    start_all(ends)
    wait_all(ends)
    opened(lax.rem(chip + step, RING) == 0, tail, pre)
    wait_all(copies)
    gates.wait()
    ups.start()

    size = length // parts

    def project(i, carry):
        branch, n = i // parts, lax.rem(i, parts)

        @pl.when(i == parts)
        def _():
            ups.wait()

        at = pl.multiple_of(n * size, 16)
        block = branch_product(xv[pl.ds(at, size), :], fv, branch, units)
        for t in range(TILES):
            part = block[:, t * 128 : min((t + 1) * 128, units)]
            pre[branch * TILES + t, pl.ds(8 + at, size), 0 : part.shape[1]] = part.astype(F32)
            end_ref[branch * TILES + t, :, 0 : part.shape[1]] = part[size - 16 :]
        return carry

    lax.fori_loop(0, 2 * parts, project, 0)
    gated(pre, taps_ref, hv)


def out_kernel(parts, table_ref, hv, *refs):
    d_refs, (own_ref, sib_ref, dv, pv, d_sems, o_sems) = refs[:RING], refs[RING:]
    core = lax.rem(table_ref[0], CORES)
    units = d_refs[0].shape[1]
    downs = Pieces(table_ref, d_refs, 0, units, dv, d_sems)
    downs.start()
    cleared(dv, units)
    downs.wait()
    size = hv.shape[0] // parts

    def product(n, carry):
        at = pl.ds(pl.multiple_of(n * size, 16), size)
        pv[at, :] = jnp.dot(hv[at, :], dv[...], preferred_element_type=F32).astype(BF16)
        return carry

    lax.fori_loop(0, parts, product, 0)
    outs = out_copies(core, pv, own_ref, sib_ref, o_sems)
    start_all(outs)
    wait_all(outs)


def widened(kept, pre):
    def step(n, carry):
        pre[n, 8:, :] = kept[n].astype(F32)
        return carry

    lax.fori_loop(0, 2 * TILES, step, 0)


def block_kernel(slot, table_ref, *refs):
    d_refs, refs = refs[:RING], refs[RING:]
    taps_ref, rows_ref, before_ref, own_ref, sib_ref, dv, kept, tail, pre, hv, pv, d_sems, p_sems, o_sems = refs
    tp = table_ref[0]
    chip, core = tp // CORES, lax.rem(tp, CORES)
    units = d_refs[0].shape[1]
    length = hv.shape[0]
    side = slot - 1
    end = before_ref if slot == 1 else before_ref.at[1, :, pl.ds(length, 16), :]
    tail_in = pltpu.make_async_copy(end, tail, p_sems.at[1])
    rows_in = pltpu.make_async_copy(rows_ref.at[side, :, pl.ds(0, length), :], kept, p_sems.at[0])
    rows_in.start()
    tail_in.start()
    downs = Pieces(table_ref, d_refs, 0, units, dv, d_sems)
    downs.start()
    cleared(dv, units)
    tail_in.wait()
    opened(lax.rem(chip + (RING - 1, 1)[side], RING) == 0, tail, pre)
    rows_in.wait()
    widened(kept, pre)
    gated(pre, taps_ref, hv)
    downs.wait()
    pv[...] = down_product(hv, dv)
    outs = out_copies(core, pv, own_ref, sib_ref, o_sems)
    start_all(outs)
    wait_all(outs)


def by_rows(rows, act):
    def step(i, carry):
        act(pl.ds(pl.multiple_of(i * 32, 32), 32))
        return carry

    lax.fori_loop(0, rows // 32, step, 0)


def add_kernel(own_ref, sib_ref, out_ref):
    def add(at):
        out_ref[at, :] = (own_ref[at, :].astype(F32) + sib_ref[at, :].astype(F32)).astype(BF16)

    by_rows(out_ref.shape[0], add)


def relay_kernel(table_ref, own_left, sib_left, own_right, sib_right, relay_ref, left_ref, right_ref):
    core = lax.rem(table_ref[0], CORES)

    def add(at):
        relay = relay_ref[at, :].astype(F32)
        left = own_left[at, :].astype(F32) + sib_left[at, :].astype(F32)
        right = own_right[at, :].astype(F32) + sib_right[at, :].astype(F32)
        left_ref[at, :] = (left + jnp.where(core == 1, relay, 0.0)).astype(BF16)
        right_ref[at, :] = (right + jnp.where(core == 0, relay, 0.0)).astype(BF16)

    by_rows(left_ref.shape[0], add)


def final_kernel(after_ref, a_ref, b_ref, c_ref, d_ref, gain_ref, out_ref):
    gain = gain_ref[...]
    chunk = 32

    def step(i, carry):
        at = pl.ds(pl.multiple_of(i * chunk, chunk), chunk)
        total = (a_ref[at, :].astype(F32) + b_ref[at, :].astype(F32)) + (c_ref[at, :].astype(F32) + d_ref[at, :].astype(F32))
        scale = lax.rsqrt(jnp.mean(total * total, axis=-1, keepdims=True) + rms_eps)
        out_ref[at, :] = (after_ref[at, :] + total * scale * gain).astype(BF16)
        return carry

    lax.fori_loop(0, after_ref.shape[0] // chunk, step, 0)


def called(kernel, out_shape, in_specs, out_specs, scratch, cost, limit):
    return pl.pallas_call(
        kernel,
        out_shape=out_shape,
        in_specs=in_specs,
        out_specs=out_specs,
        scratch_shapes=scratch,
        cost_estimate=cost,
        compiler_params=pltpu.CompilerParams(vmem_limit_bytes=limit * 2**20),
    )


def cost(flops, size):
    return pl.CostEstimate(flops=int(flops), bytes_accessed=int(size), transcendentals=0)


def shards(
    tokens,
    mix_gain_in,
    pool_weight,
    mix_gain_out,
    ffn_gain_in,
    gate_weight,
    up_weight,
    gate_taps,
    up_taps,
    down_weight,
    ffn_gain_out,
):
    rows, features = tokens.shape
    groups, part, width = pool_weight.shape
    units = gate_weight.shape[1]
    table = table_of()

    half = groups // CORES
    mine, piece, end = called(
        prepare_kernel,
        (
            jax.ShapeDtypeStruct((half, part, width), BF16),
            jax.ShapeDtypeStruct((2 * units, down_weight.shape[1]), BF16),
            jax.ShapeDtypeStruct((HALO, features), BF16),
        ),
        [whole(pltpu.SMEM)] + [whole(pltpu.HBM)] * 4,
        (whole(),) * 3,
        [pltpu.SemaphoreType.DMA((4,))],
        cost(1e8, 1e6),
        60,
    )(table, pool_weight, gate_weight.T, up_weight.T, tokens)
    halo = sent(end, NEXT_ROWS)
    lines = gathered_lines(mine)
    others = [sent(a, SWAP) for a in lines]
    pieces = gathered_lines(piece)
    downs = gathered_lines(down_weight)

    gap, taps = called(
        gap_kernel,
        (
            jax.ShapeDtypeStruct((rows, features), BF16),
            jax.ShapeDtypeStruct((gate_taps.shape[0], 2 * TILES * 128), F32),
        ),
        [whole(pltpu.SMEM)] + [whole()] * 5,
        (whole(), whole()),
        [pltpu.VMEM((rows + HALO, features), F32)],
        cost(3e9, 1.6e6),
        8,
    )(table, tokens, halo, mix_gain_in.reshape(1, features), gate_taps, up_taps)

    part_shape = jax.ShapeDtypeStruct((rows, features), BF16)
    after, channel = called(
        mix_kernel,
        (jax.ShapeDtypeStruct((rows, features), F32), part_shape),
        [whole(pltpu.SMEM), whole(), whole()] + [whole(pltpu.HBM)] * 8 + [whole(), whole()],
        (whole(), whole()),
        [
            pltpu.VMEM((groups, width, width), BF16),
            pltpu.VMEM((rows, features), BF16),
            pltpu.SemaphoreType.DMA((2 * RING * RING,)),
        ],
        cost(4e9, 6e6),
        12,
    )(table, gap, tokens, *lines, *others, mix_gain_out.reshape(1, features), ffn_gain_in.reshape(1, features))

    one, two = sent(channel, X_ONE), sent(channel, X_TWO)
    far = sent(one, X_ONE)
    here2, one2, two2, far2 = (sent(a, SWAP) for a in (channel, one, two, far))

    chip_length = CORES * rows
    fv = pltpu.VMEM((2 * units, features), BF16)
    dv = pltpu.VMEM((TILES * 128, features), BF16)
    sems = pltpu.SemaphoreType.DMA
    flops_in = 2 * chip_length * features * 2 * units
    flops_out = flops_in / 2

    pre = called(
        project_kernel,
        jax.ShapeDtypeStruct((2, 2 * TILES, chip_length + HALO, 128), BF16),
        [whole(pltpu.SMEM)] + [whole(pltpu.HBM)] * 10,
        whole(pltpu.HBM),
        [
            pltpu.VMEM((2, chip_length + HALO, features), BF16),
            fv,
            pltpu.VMEM((2, 2 * TILES, chip_length + HALO, 128), BF16),
            sems((6,)),
            sems((2, 16)),
            sems((2, 2)),
        ],
        cost(flops_in * 2, 1.2e7),
        24,
    )(table, channel, here2, one, one2, two, two2, *pieces)
    row_block = pltpu.VMEM((chip_length, features), BF16)
    kept_block = pltpu.VMEM((2 * TILES, chip_length, 128), BF16)
    pre_block = pltpu.VMEM((2 * TILES, chip_length + 8, 128), F32)
    tail_block = pltpu.VMEM((2 * TILES, 16, 128), BF16)
    hidden_block = pltpu.VMEM((chip_length, TILES * 128), BF16)

    def hidden_of(step, before, parts, own_x, sib_x):
        return called(
            functools.partial(last_kernel, step, before, parts),
            (
                jax.ShapeDtypeStruct((chip_length, TILES * 128), BF16),
                jax.ShapeDtypeStruct((2 * TILES, 16, 128), BF16),
            ),
            [whole(pltpu.SMEM)] + [whole(pltpu.HBM)] * 6 + [whole(), whole(pltpu.HBM)],
            (whole(), whole()),
            [row_block, fv, pre_block, tail_block, sems((2,)), sems((2, 16)), sems((1,))],
            cost(flops_in, 1.2e7),
            24,
        )(table, own_x, sib_x, *pieces, taps, pre)

    def out_of(parts, hidden):
        return called(
            functools.partial(out_kernel, parts),
            (part_shape, part_shape),
            [whole(pltpu.SMEM), whole()] + [whole(pltpu.HBM)] * 4,
            (whole(), whole(pltpu.HBM)),
            [dv, row_block, sems((16,)), sems((2,))],
            cost(flops_out, 6e6),
            14,
        )(table, hidden, *downs)

    hidden_far, end_far = hidden_of(2, 1, 1, far, far2)
    own_far, sib_far = out_of(1, hidden_far)
    sum_far = called(
        add_kernel, part_shape, [whole(), whole()], whole(), [], cost(1e8, 3e6), 8
    )(own_far, sent(sib_far, SWAP))
    relay = sent(sum_far, X_ONE)

    def block(slot, rows_kept, before):
        return called(
            functools.partial(block_kernel, slot),
            (part_shape, part_shape),
            [whole(pltpu.SMEM)] + [whole(pltpu.HBM)] * 4 + [whole()] + [whole(pltpu.HBM)] * 2,
            (whole(), whole(pltpu.HBM)),
            [dv, kept_block, tail_block, pre_block, hidden_block, row_block, sems((16,)), sems((2,)), sems((2,))],
            cost(flops_out, 6e6),
            22,
        )(table, *downs, taps, rows_kept, before)

    own_left, sib_left = block(1, pre, end_far)
    sib_left = sent(sib_left, SWAP)
    own_right, sib_right = block(2, pre, pre)
    sum_left, sum_right = called(
        relay_kernel,
        (part_shape, part_shape),
        [whole(pltpu.SMEM)] + [whole()] * 5,
        (whole(), whole()),
        [],
        cost(2e8, 6e6),
        8,
    )(table, own_left, sib_left, own_right, sent(sib_right, SWAP), relay)
    got_left = sent(sum_right, X_UP)
    got_right = sent(sum_left, X_DOWN)
    hidden_here, _ = hidden_of(0, 0, PARTS, channel, here2)
    own_here, sib_here = out_of(PARTS, hidden_here)
    got_here = sent(sib_here, SWAP)
    return called(
        final_kernel, part_shape, [whole()] * 6, whole(), [], cost(2e9, 6e6), 12
    )(after, own_here, got_here, got_left, got_right, ffn_gain_out.reshape(1, features))


def solution(mesh):
    in_specs = (
        P(("rep", "fs", "tp"), None),
        P(),
        P(None, "fs", None),
        P(),
        P(),
        P("fs", "tp"),
        P("fs", "tp"),
        P(),
        P(),
        P("tp", "fs"),
        P(),
    )
    out_specs = P(("rep", "fs", "tp"), None)

    return jax.shard_map(shards, mesh=mesh, in_specs=in_specs, out_specs=out_specs, check_vma=False)
```
